512 devices in a mesh: sp: 64 (over z, y), fs: 4 (over x), tp: 2 (over core).
Axes of the slice: x: 4, y: 8, z: 8, core: 2. Of those that a mesh axis runs over, the one named last changes fastest.
Arguments:
- tokens: bfloat16 [16384, 2048], P(('sp', 'fs', 'tp')), may hold values from -20 to 20
- norm_gain: float32 [2048], replicated, may hold values from 0.1 to 1.9
- query_weight: bfloat16 [2048, 1024], P(None, ('fs', 'tp')), may hold values from -0.5 to 0.5
- w_key: bfloat16 [2048, 256], P(None, 'tp'), may hold values from -0.5 to 0.5
- w_value: bfloat16 [2048, 256], P(None, 'tp'), may hold values from -0.125 to 0.125
- w_input: bfloat16 [2048, 1024], P(None, ('fs', 'tp')), may hold values from -0.125 to 0.125
- w_gate: bfloat16 [2048, 1024], P(None, ('fs', 'tp')), may hold values from -0.125 to 0.125
- conv_kernel: float32 [4, 1024], P(None, ('fs', 'tp')), may hold values from -3 to 3
- w_recur: bfloat16 [16, 64, 64], P(('fs', 'tp')), may hold values from -0.75 to 0.75
- w_admit: bfloat16 [16, 64, 64], P(('fs', 'tp')), may hold values from -0.75 to 0.75
- decay_param: float32 [1024], P(('fs', 'tp')), may hold values from 4 to 17
- decay_scale: float32 [16384, 1024], P('sp', ('fs', 'tp')), may hold values from 0.5 to 229376
- init_state: float32 [1024], P(('fs', 'tp')), may hold values from -6 to 6
- diff_lambda: float32 [8], P(('fs', 'tp')), may hold values from 0.3 to 0.8
- head_gain: float32 [128], replicated, may hold values from 0.1 to 1.9
- w_out_lru: bfloat16 [1024, 2048], P(('fs', 'tp')), may hold values from -1 to 1
- w_out_attn: bfloat16 [1024, 2048], P(('fs', 'tp')), may hold values from -0.1875 to 0.1875
Outputs:
- mixed: bfloat16 [16384, 2048], P(('sp', 'fs', 'tp'))
The draws below stay inside these ranges and needn't reach their ends.
All inputs are finite; a program needn't handle non-finite values.
Results may differ from the reference program's by a relative error of at most 0.019.
Values may be sent and summed in bfloat16 or wider, within the bound.
A program may use at most 64 MiB of HBM per device.

```python
import math
import jax
import jax.numpy as jnp
from jax import lax

D = 2048
W = 1024
BD = 64
BLOCKS = 16
HEADS = 8
KV_HEADS = 2
E = 64
V = 128
CONV = 4
TOK_DEV = 256
TOKEN_SPAN = 16384
N_FS = 4
N_TP = 2


def channel_rates(key):
    base = jax.random.fold_in(key, 11)
    key_pick, key_slow, key_fast = jax.random.split(base, 3)
    share = 0.5
    slow = jax.random.uniform(key_pick, (W,), jnp.float32) < share
    slow_rate = jnp.exp(jax.random.uniform(key_slow, (W,), jnp.float32, jnp.log(0.05), jnp.log(0.25))) / (4.0 * TOKEN_SPAN)
    fast_rate = jnp.exp(jax.random.uniform(key_fast, (W,), jnp.float32, jnp.log(0.01), jnp.log(0.033))) / 4.0
    return jnp.where(slow, slow_rate, fast_rate)


def draw_decay_param(key, part):
    rates = channel_rates(key)
    return jnp.clip(-jnp.log(jnp.expm1(rates)), 4.0, 17.0)


def draw_decay_scale(key, part):
    rates = channel_rates(key)
    base = jax.random.fold_in(key, 23)
    key_block, key_spot, key_loss = jax.random.split(base, 3)
    block_count = TOKEN_SPAN // TOK_DEV
    factor = jnp.exp(jax.random.uniform(key_block, (block_count, W), jnp.float32, jnp.log(0.5), jnp.log(2.0)))
    dispersed_numbers = jnp.repeat(factor, TOK_DEV, axis=0)
    spots = jax.random.randint(key_spot, (2,), 0, TOKEN_SPAN)
    losses = jax.random.uniform(key_loss, (2, W), jnp.float32, 0.2, 0.5)
    stride_displacements = -jnp.log1p(-losses) / (4.0 * rates[None, :])
    selected_members = (jnp.arange(TOKEN_SPAN)[:, None] == spots[None, :]).astype(jnp.float32)
    clustered_numbers = jnp.dot(selected_members, stride_displacements)
    masked_elements = jnp.sum(selected_members, axis=1) > 0.0
    return jnp.clip(jnp.where(masked_elements[:, None], clustered_numbers, dispersed_numbers), 0.5, 14.0 * TOKEN_SPAN)


def first_block_lean(key, values, row_scale):
    lean_key = jax.random.fold_in(key, 43)
    common = jax.random.normal(lean_key, (D,), jnp.float32)
    common = common / jnp.sqrt(jnp.sum(common * common))
    leaning = (jnp.arange(TOKEN_SPAN) < TOK_DEV)[:, None]
    blended = 0.71 * values + 0.7 * D ** 0.5 * row_scale * common[None, :]
    return jnp.where(leaning, blended, values)


def draw_tokens(key, part):
    base = jax.random.fold_in(key, 41)
    key_body, key_rows = jax.random.split(base, 2)
    row_scale = jnp.exp(jax.random.uniform(key_rows, (TOKEN_SPAN, 1), jnp.float32, jnp.log(0.3), jnp.log(3.0)))
    values = jax.random.normal(key_body, (TOKEN_SPAN, D), jnp.float32) * row_scale
    values = first_block_lean(key, values, row_scale)
    return jnp.clip(values, -20.0, 20.0).astype(jnp.bfloat16)


def draw_query_weight(key, part):
    base = jax.random.fold_in(key, 31)
    dispersed_numbers = (2.0 / D) ** 0.5
    values = jax.random.normal(base, (D, HEADS * 2 * E), jnp.float32) * dispersed_numbers
    return jnp.clip(values, -0.5, 0.5).astype(jnp.bfloat16)


def draw_w_key(key, part):
    base = jax.random.fold_in(key, 37)
    dispersed_numbers = (1.5 / D) ** 0.5
    values = jax.random.normal(base, (D, KV_HEADS * 2 * E), jnp.float32) * dispersed_numbers
    return jnp.clip(values, -0.5, 0.5).astype(jnp.bfloat16)


def block_levels(rng, dims, pieces, least, high):
    loudness = 1.0
    for axis_at, parts in pieces:
        heights = jax.random.uniform(jax.random.fold_in(jax.random.fold_in(rng, 6), axis_at), (parts,), jnp.float32, least / len(pieces), high / len(pieces))
        loudness = loudness * jnp.repeat(jnp.exp(heights), dims[axis_at] // parts).reshape((-1,) + (1,) * (len(dims) - 1 - axis_at))
    return loudness


def scatter_about(stream_key, dims, scale, most, cuts=(), kind=jnp.bfloat16):
    drawn = jax.random.normal(stream_key, dims, jnp.float32) * scale
    if len(cuts) > 0:
        drawn = block_levels(stream_key, dims, cuts, -0.22, 0.18) * drawn
    return jnp.clip(drawn, min=-most, max=most).astype(kind)


def setup_inputs(seed: int = 0) -> dict:
    arg_keys = jax.random.split(jax.random.key(seed), 18)
    return {
        "tokens": draw_tokens(jax.random.fold_in(arg_keys[17], 71), 0),
        "norm_gain": jnp.clip(1.0 + 0.18 * jax.random.normal(arg_keys[1], (D,), jnp.float32), 0.1, 1.9),
        "query_weight": draw_query_weight(jax.random.fold_in(arg_keys[17], 71), 0),
        "w_key": draw_w_key(jax.random.fold_in(arg_keys[17], 71), 0),
        "w_value": scatter_about(arg_keys[4], (D, V * KV_HEADS), D ** -0.5, 0.125, ((1, 2),)),
        "w_input": scatter_about(arg_keys[5], (D, W), D ** -0.5, 0.125, ((1, 8),)),
        "w_gate": scatter_about(arg_keys[6], (D, W), D ** -0.5, 0.125, ((1, 8),)),
        "conv_kernel": scatter_about(arg_keys[7], (CONV, W), CONV ** -0.5, 3.0, ((1, 8),), jnp.float32),
        "w_recur": scatter_about(arg_keys[8], (BLOCKS, BD, BD), BD ** -0.5, 0.75, ((0, 8),)),
        "w_admit": scatter_about(arg_keys[9], (BLOCKS, BD, BD), BD ** -0.5, 0.75, ((0, 8),)),
        "decay_param": draw_decay_param(jax.random.fold_in(arg_keys[17], 71), 0),
        "decay_scale": draw_decay_scale(jax.random.fold_in(arg_keys[17], 71), 0),
        "init_state": scatter_about(arg_keys[12], (W,), 1.0, 6.0, ((0, 8),), jnp.float32),
        "diff_lambda": jnp.clip(0.3 + 0.5 * jax.random.uniform(arg_keys[13], (HEADS,), jnp.float32) ** block_levels(arg_keys[13], (HEADS,), ((0, 8),), -0.2, 0.2), 0.3, 0.8),
        "head_gain": jnp.clip(1.0 + 0.18 * jax.random.normal(arg_keys[14], (V,), jnp.float32), 0.1, 1.9),
        "w_out_lru": scatter_about(arg_keys[15], (W, D), (W // 32) ** -0.5, 1.0, ((0, 8),)),
        "w_out_attn": scatter_about(arg_keys[16], (HEADS * V, D), (HEADS * V) ** -0.5, 0.1875, ((0, 8),)),
    }


gate_scale = 8.0
input_eps = 1e-06
head_eps = 1e-05

def pair_combine(earlier, later):
    decay_early, state_early = earlier
    decay_late, state_late = later
    return (decay_early * decay_late, decay_late * state_early + state_late)

def project(normed, weight):
    return jnp.dot(normed, weight, preferred_element_type=jnp.float32).astype(jnp.bfloat16)

def reference(tokens, norm_gain, query_weight, w_key, w_value, w_input, w_gate, conv_kernel, w_recur, w_admit, decay_param, decay_scale, init_state, diff_lambda, head_gain, w_out_lru, w_out_attn):
    floats = tokens.astype(jnp.float32)
    normed = (floats * lax.rsqrt(lax.optimization_barrier(jnp.mean(floats * floats, axis=1, keepdims=True)) + input_eps) * norm_gain).astype(jnp.bfloat16)
    query = project(normed, query_weight)
    keys_all = project(normed, w_key)
    values_all = project(normed, w_value)
    lru_in = project(normed, w_input)
    gate_proj = project(normed, w_gate)
    padded = jnp.concatenate([jnp.zeros((CONV - 1, W), jnp.bfloat16), lru_in], axis=0).astype(jnp.float32)
    conv_sum = jnp.zeros((TOKEN_SPAN, W), jnp.float32)
    for offset in range(CONV):
        conv_sum = conv_sum + conv_kernel[offset] * padded[offset:offset + TOKEN_SPAN]
    conv_out = conv_sum.astype(jnp.bfloat16)
    grouped = conv_out.astype(jnp.float32).reshape(TOKEN_SPAN, BLOCKS, BD)
    recur = jax.nn.sigmoid(jnp.einsum('tni,nij->tnj', grouped, w_recur.astype(jnp.float32)).reshape(TOKEN_SPAN, W))
    admit = jax.nn.sigmoid(jnp.einsum('tni,nij->tnj', grouped, w_admit.astype(jnp.float32)).reshape(TOKEN_SPAN, W))
    log_decay = -gate_scale * recur * jax.nn.softplus(-decay_param) * decay_scale
    decay = jnp.exp(log_decay)
    drive = jnp.sqrt(-jnp.expm1(2.0 * log_decay)) * admit * conv_out.astype(jnp.float32)
    drive = jnp.concatenate([drive[:1] + decay[:1] * init_state[None, :], drive[1:]], axis=0)
    _, states = lax.associative_scan(pair_combine, (decay, drive), axis=0)
    lru_out = (states * jax.nn.gelu(gate_proj.astype(jnp.float32))).astype(jnp.bfloat16)
    query_heads = query.reshape(TOKEN_SPAN, HEADS, 2, E).astype(jnp.float32)
    head_owner = (jnp.arange(HEADS) % KV_HEADS).astype(jnp.int32)
    key_heads = keys_all.reshape(TOKEN_SPAN, KV_HEADS, 2, E).astype(jnp.float32)[:, head_owner]
    value_heads = values_all.reshape(TOKEN_SPAN, KV_HEADS, V).astype(jnp.float32)[:, head_owner]
    query_rows = math.gcd(TOKEN_SPAN, 256)
    key_index = jnp.arange(TOKEN_SPAN).astype(jnp.int32)

    def attend_block(block_index):
        first_row = (block_index * query_rows).astype(jnp.int32)
        block = lax.dynamic_slice_in_dim(query_heads, first_row, query_rows, 0)
        scores = jnp.einsum('qhme,khme->hmqk', block, key_heads) * E ** (-0.5)
        query_index = first_row + jnp.arange(query_rows).astype(jnp.int32)
        visible = key_index[None, :] <= query_index[:, None]
        scores = jnp.where(visible, scores, -jnp.inf)
        peak = lax.optimization_barrier(jnp.max(scores, axis=-1, keepdims=True))
        expos = jnp.where(visible, jnp.exp(scores - peak), 0.0)
        total = lax.optimization_barrier(jnp.sum(expos, axis=-1))
        weights = lax.optimization_barrier(expos.astype(jnp.bfloat16)).astype(jnp.float32)
        heads_values = jnp.einsum('hmqk,khv->hmqv', weights, value_heads)
        lam = diff_lambda[:, None, None]
        diff = heads_values[:, 0] / total[:, 0, :, None] - lam * heads_values[:, 1] / total[:, 1, :, None]
        scaled = diff * lax.rsqrt(lax.optimization_barrier(jnp.mean(diff * diff, axis=-1, keepdims=True)) + head_eps) * head_gain
        return jnp.transpose(scaled, (1, 0, 2)).reshape(query_rows, HEADS * V).astype(jnp.bfloat16)
    attn_out = lax.map(attend_block, jnp.arange(TOKEN_SPAN // query_rows).astype(jnp.int32))
    attn_out = attn_out.reshape(TOKEN_SPAN, HEADS * V)
    group_count = N_FS * N_TP
    lru_cols = W // group_count
    head_cols = HEADS * V // group_count
    mixed = jnp.zeros((TOKEN_SPAN, D), jnp.float32)
    for group_index in range(group_count):
        low = group_index * lru_cols
        high = group_index * head_cols
        partial_sum = jnp.dot(lru_out[:, low:low + lru_cols], w_out_lru[low:low + lru_cols], preferred_element_type=jnp.float32)
        partial_sum = partial_sum + jnp.dot(attn_out[:, high:high + head_cols], w_out_attn[high:high + head_cols], preferred_element_type=jnp.float32)
        rounded = lax.optimization_barrier(partial_sum.astype(jnp.bfloat16))
        mixed = mixed + rounded.astype(jnp.float32)
    return mixed.astype(jnp.bfloat16)
```

```python
import functools
import math

import jax
import jax.numpy as jnp
from jax import lax
from jax.experimental import pallas as pl
from jax.experimental.pallas import tpu as pltpu
from jax.sharding import Mesh
from jax.sharding import PartitionSpec as P

SP = ("sp_0", "sp_1")
SP_FS_TP = ("sp_0", "sp_1", "fs", "tp")
MESH = pl.DeviceIdType.MESH
BF = jnp.bfloat16
F32 = jnp.float32

gate_scale = 8.0
input_eps = 1e-06
head_eps = 1e-05
far_below = -1e30


def remote(src, dst, send, recv, where):
    return pltpu.make_async_remote_copy(
        src_ref=src, dst_ref=dst, send_sem=send, recv_sem=recv,
        device_id=where, device_id_type=MESH,
    )


def greet(peers):
    barrier = pltpu.get_barrier_semaphore()
    for peer in peers:
        pl.semaphore_signal(barrier, inc=1, device_id=peer, device_id_type=MESH)
    pl.semaphore_wait(barrier, len(peers))


def project_kernel(q_scale, tok, gain, wq, wk, wv, wi, wg, q_out, kv_out, lru_out, gate_out,
                   xbuf, nbuf, wbuf, wsem, tsem, ssem, rsem):
    x, c = lax.axis_index("fs"), lax.axis_index("tp")
    left, right, opp = lax.rem(x + 3, 4), lax.rem(x + 1, 4), lax.rem(x + 2, 4)
    rows = tok.shape[0]
    half = rows // 2
    me = 2 * x + c
    weights = [
        pltpu.make_async_copy(w, wbuf.at[:, pl.ds(128 * i, 128)], wsem.at[i])
        for i, w in enumerate((wq, wk, wv, wi, wg))
    ]
    mine = pltpu.make_async_copy(tok, xbuf.at[me], tsem)
    mine.start()
    for copy in weights:
        copy.start()
    greet([{"tp": 1 - c}, {"fs": left}, {"fs": right}])
    mine.wait()

    def piece(chip, core, part):
        ref = xbuf.at[2 * chip + core]
        if part is None:
            return ref
        return ref.at[pl.ds(part * half, half)]

    started = []

    def send(k, chip, core, part, where):
        ref = piece(chip, core, part)
        copy = remote(ref, ref, ssem.at[k], rsem.at[k], where)
        copy.start()
        started.append(copy)

    def arrive(k, chip, core, part):
        ref = piece(chip, core, part)
        remote(ref, ref, ssem.at[k], rsem.at[k], {"tp": 1 - c}).wait_recv()

    def norm(chip, core):
        slot = 2 * chip + core
        t = xbuf[slot].astype(F32)
        ms = jnp.mean(t * t, axis=1, keepdims=True)
        nbuf[pl.ds(pl.multiple_of(slot * rows, rows), rows), :] = (
            t * lax.rsqrt(ms + input_eps) * gain[...]
        ).astype(BF)

    sib = {"tp": 1 - c}
    to_right, to_left = {"fs": right}, {"fs": left}
    send(1, x, c, 0, to_right)
    send(3, x, c, 1, to_left)
    send(2, x, c, 1, to_right)
    send(4, x, c, 0, to_left)
    send(0, x, c, None, sib)
    norm(x, c)
    arrive(0, x, 1 - c, None)
    norm(x, 1 - c)
    arrive(1, left, c, 0)
    send(5, left, c, 0, to_right)
    send(7, left, c, 0, sib)
    arrive(3, right, c, 1)
    send(6, right, c, 1, to_left)
    send(9, right, c, 1, sib)
    arrive(2, left, c, 1)
    send(8, left, c, 1, sib)
    arrive(4, right, c, 0)
    send(10, right, c, 0, sib)
    norm(left, c)
    norm(right, c)
    arrive(7, left, 1 - c, 0)
    arrive(8, left, 1 - c, 1)
    norm(left, 1 - c)
    arrive(9, right, 1 - c, 1)
    arrive(10, right, 1 - c, 0)
    norm(right, 1 - c)
    arrive(5, opp, c, 0)
    send(11, opp, c, 0, sib)
    arrive(6, opp, c, 1)
    send(12, opp, c, 1, sib)
    norm(opp, c)
    for copy in weights:
        copy.wait()
    arrive(11, opp, 1 - c, 0)
    arrive(12, opp, 1 - c, 1)
    norm(opp, 1 - c)
    both = jnp.dot(nbuf[...], wbuf[...], preferred_element_type=F32)
    q_out[...] = (both[:, 0:128] * q_scale).astype(BF)
    kv_out[...] = both[:, 128:384].astype(BF)
    lru_out[...] = both[:, 384:512].astype(BF)
    gate_out[...] = both[:, 512:640].astype(BF)
    for copy in started:
        copy.wait_send()


def project_call(tokens, gain, wq, wk, wv, wi, wg):
    rows, d = tokens.shape
    whole = rows * 8
    vm = pl.BlockSpec(memory_space=pltpu.VMEM)
    hb = pl.BlockSpec(memory_space=pl.ANY)
    size_qk = wq.shape[1] // 2
    q_scale = size_qk ** (-0.5) * math.log2(math.e)
    return pl.pallas_call(
        functools.partial(project_kernel, q_scale),
        out_shape=[
            jax.ShapeDtypeStruct((whole, 128), BF),
            jax.ShapeDtypeStruct((whole, 256), BF),
            jax.ShapeDtypeStruct((whole, 128), BF),
            jax.ShapeDtypeStruct((whole, 128), BF),
        ],
        in_specs=[hb, vm] + [hb] * 5,
        out_specs=[vm] * 4,
        scratch_shapes=[
            pltpu.VMEM((8, rows, d), BF),
            pltpu.VMEM((whole, d), BF),
            pltpu.VMEM((d, 640), BF),
            pltpu.SemaphoreType.DMA((5,)),
            pltpu.SemaphoreType.DMA,
            pltpu.SemaphoreType.DMA((13,)),
            pltpu.SemaphoreType.DMA((13,)),
        ],
        compiler_params=pltpu.CompilerParams(collective_id=0, has_side_effects=True),
        name="project",
    )(tokens, gain.reshape(1, d), wq, wk, wv, wi, wg)


def scan_rows(a, b, rows):
    row = lax.broadcasted_iota(jnp.int32, a.shape, 0)
    d = 1
    while d < rows:
        a_early = jnp.where(row >= d, pltpu.roll(a, d, axis=0), 1.0)
        b_early = jnp.where(row >= d, pltpu.roll(b, d, axis=0), 0.0)
        b = a * b_early + b
        a = a * a_early
        d *= 2
    return a, b


def log1p_small(u):
    s = u / (2.0 + u)
    s2 = s * s
    total = jnp.full_like(s, 1.0 / 15.0)
    for k in (13, 11, 9, 7, 5, 3, 1):
        total = total * s2 + 1.0 / k
    return 2.0 * s * total


def minus_expm1(v):
    series = jnp.full_like(v, 1.0 / 11.0)
    total = 1.0 + v * series
    for k in (10, 9, 8, 7, 6, 5, 4, 3, 2):
        total = 1.0 + v * total * (1.0 / k)
    return jnp.where(v > -0.5, -v * total, 1.0 - jnp.exp(v))


def gelu(v):
    return 0.5 * v * (1.0 + jnp.tanh(math.sqrt(2.0 / math.pi) * (v + 0.044715 * v * v * v)))


def fold_pairs(buf, here, n):
    a_in = jnp.ones((1, 128), F32)
    b_in = jnp.zeros((1, 128), F32)
    a_all, b_all = a_in, b_in
    for k in range(n):
        a, b = buf[k, 0:1, :], buf[k, 1:2, :]
        a_all, b_all = a_all * a, a * b_all + b
        past = k < here
        a_in, b_in = jnp.where(past, a_all, a_in), jnp.where(past, b_all, b_in)
    return a_in, b_in, a_all, b_all


def mix_kernel(q_ref, kv_ref, lru_in, gate, taps, w_recur, w_admit, param, scale, init,
               o_ref, lse_ref, lru_out,
               kva, kvb, qbuf, qp, m_s, l_s, acc, bias_s, halo, pad, wgate, run_a, run_b, ab_y, ab_z, ab_me, lse_s,
               q_ss, q_rs, p_ss, p_rs, r_ss, r_rs, h_ss, h_rs, ab_ss, ab_rs):
    z, y = lax.axis_index("sp_0"), lax.axis_index("sp_1")
    x, c = lax.axis_index("fs"), lax.axis_index("tp")
    left, right, opp = lax.rem(x + 3, 4), lax.rem(x + 1, 4), lax.rem(x + 2, 4)
    n = 8

    def wrap(v):
        return lax.rem(v + 2 * n, n)

    sp = z * n + y
    after, before = lax.rem(sp + 1, 64), lax.rem(sp + 63, 64)
    nxt = {"sp_0": after // n, "sp_1": lax.rem(after, n)}
    prev = {"sp_0": before // n, "sp_1": lax.rem(before, n)}
    greet(
        [{"sp_1": wrap(y + d)} for d in range(1, n)]
        + [{"sp_0": wrap(z + d)} for d in range(1, n)]
        + [{"fs": left}, {"fs": right}, nxt, prev]
    )
    started = []

    def go(src, dst, ss, rs, where):
        copy = remote(src, dst, ss, rs, where)
        copy.start()
        started.append(copy)

    def took(dst, ss, rs, where):
        remote(dst, dst, ss, rs, where).wait_recv()

    def part(ref, i, at, size):
        return ref.at[i, pl.ds(pl.multiple_of(at, 32), size), :]

    base = x * 64
    src_a = kv_ref.at[pl.ds(pl.multiple_of(base, 32), 32), :]
    src_b = kv_ref.at[pl.ds(pl.multiple_of(base + 32, 32), 32), :]
    for d in (1, 7, 2, 6, 3, 5, 4):
        go(src_a, part(kva, z, y * 32, 32), p_ss.at[0, d], p_rs.at[0, d], {"sp_1": wrap(y + d)})
        go(src_b, part(kvb, y, z * 32, 32), p_ss.at[1, d], p_rs.at[1, d], {"sp_0": wrap(z + d)})
    rows = q_ref.shape[0]
    half = rows // 2

    def q_src(h):
        return q_ref.at[pl.ds(h * half, half), :]

    def q_at(chip, h):
        return qbuf.at[chip, pl.ds(h * half, half), :]

    to_right, to_left = {"fs": right}, {"fs": left}
    go(q_src(0), q_at(x, 0), q_ss.at[0], q_rs.at[0], to_right)
    go(q_src(1), q_at(x, 1), q_ss.at[1], q_rs.at[1], to_left)
    go(q_src(1), q_at(x, 1), q_ss.at[2], q_rs.at[2], to_right)
    go(q_src(0), q_at(x, 0), q_ss.at[3], q_rs.at[3], to_left)
    go(lru_in.at[pl.ds(rows - 16, 16), :], halo, h_ss, h_rs, nxt)

    kva[z, pl.ds(pl.multiple_of(y * 32, 32), 32), :] = kv_ref[pl.ds(pl.multiple_of(base, 32), 32), :]
    kvb[y, pl.ds(pl.multiple_of(z * 32, 32), 32), :] = kv_ref[pl.ds(pl.multiple_of(base + 32, 32), 32), :]

    row = lax.broadcasted_iota(jnp.int32, (rows, 256), 0)
    lane = lax.broadcasted_iota(jnp.int32, (rows, 256), 1)
    block, inner = lane // 32, lax.rem(lane, 32)
    q_pos = sp * rows + row
    key_a = (z * n + block) * rows + base + inner
    key_b = (block * n + y) * rows + base + 32 + inner
    bias_s[0] = jnp.where(key_a <= q_pos, 0.0, far_below)
    bias_s[1] = jnp.where(key_b <= q_pos, 0.0, far_below)

    first_lanes = lax.broadcasted_iota(jnp.int32, (rows, 128), 1) < 64

    def ready_q(chip, value):
        v = value.astype(F32)
        qp[2 * chip] = jnp.where(first_lanes, v, 0.0).astype(BF)
        qp[2 * chip + 1] = jnp.where(first_lanes, 0.0, v).astype(BF)

    ready_q(x, q_ref[...])
    took(q_at(left, 0), q_ss.at[0], q_rs.at[0], to_left)
    go(q_at(left, 0), q_at(left, 0), q_ss.at[4], q_rs.at[4], to_right)
    took(q_at(right, 1), q_ss.at[1], q_rs.at[1], to_right)
    go(q_at(right, 1), q_at(right, 1), q_ss.at[5], q_rs.at[5], to_left)

    def ring(which, buf, axis, me):
        up, down = {axis: wrap(me + 1)}, {axis: wrap(me - 1)}

        def half_of(i, h):
            return part(buf, i, h * 128, 128)

        def hop(s, h, direction):
            origin = wrap(me - (s - 1)) if direction == 0 else wrap(me + (s - 1))
            k = (which, direction, s - 1, h)
            go(half_of(origin, h), half_of(origin, h), r_ss.at[k], r_rs.at[k], up if direction == 0 else down)

        def land(s, h, direction):
            origin = wrap(me - s) if direction == 0 else wrap(me + s)
            k = (which, direction, s - 1, h)
            took(half_of(origin, h), r_ss.at[k], r_rs.at[k], down if direction == 0 else up)

        return hop, land

    hop_a, land_a = ring(0, kva, "sp_0", z)
    hop_b, land_b = ring(1, kvb, "sp_1", y)
    for d in range(1, n):
        took(part(kva, z, wrap(y - d) * 32, 32), p_ss.at[0, d], p_rs.at[0, d], {"sp_1": wrap(y - d)})
        took(part(kvb, y, wrap(z - d) * 32, 32), p_ss.at[1, d], p_rs.at[1, d], {"sp_0": wrap(z - d)})
    for h in (0, 1):
        for direction in (0, 1):
            hop_a(1, h, direction)
            hop_b(1, h, direction)

    took(halo, h_ss, h_rs, prev)
    pad[0:8, :] = jnp.where(sp > 0, halo[8:16, :].astype(F32), 0.0)
    pad[8:8 + rows, :] = lru_in[...].astype(F32)
    conv = jnp.zeros((rows, 128), F32)
    for j in range(4):
        conv = conv + taps[j:j + 1, :] * pad[5 + j:5 + j + rows, :]
    conv_bf = conv.astype(BF)
    wgate[...] = jnp.zeros_like(wgate)
    for i, w in enumerate((w_recur, w_admit)):
        zero = jnp.zeros((64, 64), F32)
        wgate[0:64, 128 * i:128 * i + 128] = jnp.concatenate([w[0].astype(F32), zero], axis=1).astype(BF)
        wgate[64:128, 128 * i:128 * i + 128] = jnp.concatenate([zero, w[1].astype(F32)], axis=1).astype(BF)
    gates = jnp.dot(conv_bf, wgate[...], preferred_element_type=F32)
    gates = 1.0 / (1.0 + jnp.exp(-gates))
    recur, admit = gates[:, :128], gates[:, 128:]
    p = param[...]
    soft = jnp.maximum(-p, 0.0) + log1p_small(jnp.exp(-jnp.abs(p)))
    log_decay = -gate_scale * recur * soft * scale[...]
    decay = jnp.exp(log_decay)
    drive = jnp.sqrt(minus_expm1(2.0 * log_decay)) * admit * conv_bf.astype(F32)
    a, b = scan_rows(decay, drive, rows)
    run_a[...] = a
    run_b[...] = b
    ab_me[0, 0:1, :] = run_a[rows - 1:rows, :]
    ab_me[0, 1:2, :] = run_b[rows - 1:rows, :]
    for d in range(1, n):
        go(ab_me.at[0], ab_y.at[y], ab_ss.at[0, d], ab_rs.at[0, d], {"sp_1": wrap(y + d)})

    took(q_at(left, 1), q_ss.at[2], q_rs.at[2], to_left)
    ready_q(left, qbuf[left])
    took(q_at(right, 0), q_ss.at[3], q_rs.at[3], to_right)
    ready_q(right, qbuf[right])
    took(q_at(opp, 0), q_ss.at[4], q_rs.at[4], to_left)
    took(q_at(opp, 1), q_ss.at[5], q_rs.at[5], to_right)
    ready_q(opp, qbuf[opp])

    nt = (((1,), (1,)), ((), ()))

    def attend(first, ia, ib, lim_a=None, lim_b=None):
        lane1 = lax.broadcasted_iota(jnp.int32, (1, 256), 1)
        if not first:
            row_a = jnp.where(lane1 < lim_a, 0.0, far_below)
            row_b = jnp.where(lane1 < lim_b, 0.0, far_below)

        def one(hm, carry):
            q = qp[hm]
            sa = lax.dot_general(q, kva[ia, :, 0:128], nt, preferred_element_type=F32)
            sb = lax.dot_general(q, kvb[ib, :, 0:128], nt, preferred_element_type=F32)
            if first:
                sa, sb = sa + bias_s[0], sb + bias_s[1]
            else:
                sa, sb = sa + row_a, sb + row_b
            parts = [sa[:, :128], sa[:, 128:], sb[:, :128], sb[:, 128:]]
            top = jnp.maximum(jnp.maximum(parts[0], parts[1]), jnp.maximum(parts[2], parts[3]))
            top = jnp.broadcast_to(jnp.max(top, axis=1, keepdims=True), (rows, 128))
            if first:
                m_new = top
            else:
                m_old = m_s[hm]
                m_new = jnp.maximum(m_old, top)
                fade = jnp.exp2(m_old - m_new)
            expos = [jnp.exp2(v - m_new) for v in parts]
            line = (expos[0] + expos[1]) + (expos[2] + expos[3])
            pa = jnp.concatenate([expos[0].astype(BF), expos[1].astype(BF)], axis=1)
            pb = jnp.concatenate([expos[2].astype(BF), expos[3].astype(BF)], axis=1)
            new = jnp.dot(pa, kva[ia, :, 128:256], preferred_element_type=F32)
            new = new + jnp.dot(pb, kvb[ib, :, 128:256], preferred_element_type=F32)
            m_s[hm] = m_new
            if first:
                l_s[hm] = line
                acc[hm] = new
            else:
                l_s[hm] = l_s[hm] * fade + line
                acc[hm] = acc[hm] * fade + new
            return carry

        lax.fori_loop(0, 8, one, 0)

    def pair(step):
        za, yb = wrap(z + step), wrap(y + step)
        lim_a = jnp.where(za < z, 256, 0)
        lim_b = (z + jnp.where(yb < y, 1, 0)) * 32

        @pl.when(jnp.logical_or(za < z, lim_b > 0))
        def _():
            attend(False, za, yb, lim_a, lim_b)

    attend(True, z, y)
    for s in (1, 2, 3):
        for h in (0, 1):
            for direction in (0, 1):
                land_a(s, h, direction)
                land_b(s, h, direction)
                if s < 3 or h == direction:
                    hop_a(s + 1, h, direction)
                    hop_b(s + 1, h, direction)
        pair(-s)
        pair(s)
        if s == 1:
            for d in range(1, n):
                took(ab_y.at[wrap(y - d)], ab_ss.at[0, d], ab_rs.at[0, d], {"sp_1": wrap(y - d)})
            ab_y[y] = ab_me[0]
            a_in, b_in, a_all, b_all = fold_pairs(ab_y, y, n)
            ab_me[1, 0:1, :] = a_all
            ab_me[1, 1:2, :] = b_all
            ab_me[2, 0:1, :] = a_in
            ab_me[2, 1:2, :] = b_in
            for d in range(1, n):
                go(ab_me.at[1], ab_z.at[z], ab_ss.at[1, d], ab_rs.at[1, d], {"sp_0": wrap(z + d)})
        if s == 3:
            for d in range(1, n):
                took(ab_z.at[wrap(z - d)], ab_ss.at[1, d], ab_rs.at[1, d], {"sp_0": wrap(z - d)})
            ab_z[z] = ab_me[1]
            a_out, b_out, _, _ = fold_pairs(ab_z, z, n)
            a_in, b_in = ab_me[2, 0:1, :], ab_me[2, 1:2, :]
            a_in, b_in = a_out * a_in, a_in * b_out + b_in
            entering = a_in * init[...] + b_in
            states = run_b[...] + run_a[...] * entering
            lru_out[...] = (states * gelu(gate[...].astype(F32))).astype(BF)
    for direction in (0, 1):
        land_a(4, direction, direction)
        land_b(4, direction, direction)
    pair(4)

    spot = lax.broadcasted_iota(jnp.int32, (rows, 128), 1)

    lse_s[...] = jnp.zeros_like(lse_s)

    def close(hm, carry):
        total = jnp.sum(l_s[hm], axis=1, keepdims=True)
        o_ref[hm] = (acc[hm] / total).astype(BF)
        lse = m_s[hm] + jnp.log(total) * math.log2(math.e)
        lse_s[...] = jnp.where(spot == hm, lse, lse_s[...])
        return carry

    lax.fori_loop(0, 8, close, 0)
    lse_ref[...] = jnp.transpose(lse_s[...])[0:8, :]
    for copy in started:
        copy.wait_send()


def mix_call(q, kv, lru_in, gate, taps, w_recur, w_admit, param, scale, init):
    rows = q.shape[0]
    vm = pl.BlockSpec(memory_space=pltpu.VMEM)
    dma = pltpu.SemaphoreType.DMA
    return pl.pallas_call(
        mix_kernel,
        out_shape=[
            jax.ShapeDtypeStruct((8, rows, 128), BF),
            jax.ShapeDtypeStruct((8, rows), F32),
            jax.ShapeDtypeStruct((rows, 128), BF),
        ],
        in_specs=[vm] * 10,
        out_specs=[vm] * 3,
        scratch_shapes=[
            pltpu.VMEM((8, 256, 256), BF),
            pltpu.VMEM((8, 256, 256), BF),
            pltpu.VMEM((4, rows, 128), BF),
            pltpu.VMEM((8, rows, 128), BF),
            pltpu.VMEM((8, rows, 128), F32),
            pltpu.VMEM((8, rows, 128), F32),
            pltpu.VMEM((8, rows, 128), F32),
            pltpu.VMEM((2, rows, 256), F32),
            pltpu.VMEM((16, 128), BF),
            pltpu.VMEM((rows + 8, 128), F32),
            pltpu.VMEM((128, 256), BF),
            pltpu.VMEM((rows, 128), F32),
            pltpu.VMEM((rows, 128), F32),
            pltpu.VMEM((8, 8, 128), F32),
            pltpu.VMEM((8, 8, 128), F32),
            pltpu.VMEM((3, 8, 128), F32),
            pltpu.VMEM((rows, 128), F32),
            dma((6,)), dma((6,)),
            dma((2, 8)), dma((2, 8)),
            dma((2, 2, 4, 2)), dma((2, 2, 4, 2)),
            dma, dma,
            dma((2, 8)), dma((2, 8)),
        ],
        compiler_params=pltpu.CompilerParams(collective_id=1, has_side_effects=True),
        name="mix",
    )(q, kv, lru_in, gate, taps, w_recur, w_admit, param.reshape(1, 128), scale, init.reshape(1, 128))


def output_kernel(o_ref, lse_ref, lru, lam, gain, w_lru, w_attn, out_ref,
                  got, relay, lses, lhs, wbuf, pbuf, sib_in, sbuf, r2, fin,
                  wsem, c_ss, c_rs, s_ss, s_rs):
    x, c = lax.axis_index("fs"), lax.axis_index("tp")
    left, right, opp = lax.rem(x + 3, 4), lax.rem(x + 1, 4), lax.rem(x + 2, 4)
    to_right, to_left, to_opp, sib = {"fs": right}, {"fs": left}, {"fs": opp}, {"tp": 1 - c}
    weights = [
        pltpu.make_async_copy(w_lru, wbuf.at[pl.ds(0, 128), :], wsem.at[0]),
        pltpu.make_async_copy(w_attn, wbuf.at[pl.ds(128, 128), :], wsem.at[1]),
    ]
    for copy in weights:
        copy.start()
    greet([sib, to_left, to_right, to_opp])
    started = []

    def go(src, dst, ss, rs, where):
        copy = remote(src, dst, ss, rs, where)
        copy.start()
        started.append(copy)

    def took(dst, ss, rs, where):
        remote(dst, dst, ss, rs, where).wait_recv()

    go(lse_ref, lses.at[2], c_ss.at[0], c_rs.at[0], to_opp)
    go(lse_ref, lses.at[0], c_ss.at[1], c_rs.at[1], to_right)
    go(lse_ref, lses.at[1], c_ss.at[2], c_rs.at[2], to_left)
    go(o_ref.at[2 * opp], relay.at[0], c_ss.at[3], c_rs.at[3], to_right)
    go(o_ref.at[2 * opp + 1], relay.at[1], c_ss.at[4], c_rs.at[4], to_left)
    go(o_ref.at[pl.ds(2 * right, 2)], got.at[0], c_ss.at[5], c_rs.at[5], to_right)
    go(o_ref.at[pl.ds(2 * left, 2)], got.at[1], c_ss.at[6], c_rs.at[6], to_left)
    took(relay.at[0], c_ss.at[3], c_rs.at[3], to_left)
    go(relay.at[0], got.at[2, 0], c_ss.at[7], c_rs.at[7], to_right)
    took(relay.at[1], c_ss.at[4], c_rs.at[4], to_right)
    go(relay.at[1], got.at[2, 1], c_ss.at[8], c_rs.at[8], to_left)
    rows = lru.shape[0]
    lhs[:, 0:128] = lru[...]
    took(lses.at[2], c_ss.at[0], c_rs.at[0], to_opp)
    took(lses.at[0], c_ss.at[1], c_rs.at[1], to_left)
    took(lses.at[1], c_ss.at[2], c_rs.at[2], to_right)

    def column(line):
        return jnp.transpose(jnp.broadcast_to(line, (128, rows)))

    heads = []
    shares = []
    for m in (0, 1):
        lines = [lse_ref[pl.ds(2 * x + m, 1), :]] + [lses[i, pl.ds(2 * x + m, 1), :] for i in range(3)]
        top = functools.reduce(jnp.maximum, lines)
        powers = [jnp.exp2(v - top) for v in lines]
        total = functools.reduce(jnp.add, powers)
        shares.append([column(v / total) for v in powers])
    took(got.at[0], c_ss.at[5], c_rs.at[5], to_left)
    took(got.at[1], c_ss.at[6], c_rs.at[6], to_right)
    took(got.at[2, 0], c_ss.at[7], c_rs.at[7], to_left)
    took(got.at[2, 1], c_ss.at[8], c_rs.at[8], to_right)
    for m in (0, 1):
        value = shares[m][0] * o_ref[2 * x + m].astype(F32)
        for i in range(3):
            value = value + shares[m][1 + i] * got[i, m].astype(F32)
        heads.append(value)
    diff = heads[0] - lam[...] * heads[1]
    ms = jnp.mean(diff * diff, axis=1, keepdims=True)
    lhs[:, 128:256] = (diff * lax.rsqrt(ms + head_eps) * gain[...]).astype(BF)
    for copy in weights:
        copy.wait()

    def make(chip, k):
        at = pl.multiple_of(chip * 64, 64)
        value = jnp.dot(lhs[pl.ds(at, 64), :], wbuf[...], preferred_element_type=F32)
        pbuf[k] = value.astype(BF).reshape(2, 32, value.shape[1])
        go(pbuf.at[k, 1 - c], sib_in.at[k], s_ss.at[k], s_rs.at[k], sib)

    def both(k):
        took(sib_in.at[k], s_ss.at[k], s_rs.at[k], sib)
        return pbuf[k, c].astype(F32) + sib_in[k].astype(F32)

    make(opp, 0)
    make(right, 1)
    make(left, 2)
    sbuf[0] = both(0).astype(BF)
    go(sbuf.at[0, pl.ds(0, 16), :], r2.at[0], s_ss.at[4], s_rs.at[4], to_right)
    go(sbuf.at[0, pl.ds(16, 16), :], r2.at[1], s_ss.at[5], s_rs.at[5], to_left)
    make(x, 3)
    sum_right, sum_left = both(1), both(2)
    sbuf[1, 16:32] = sum_right[16:32].astype(BF)
    sbuf[2, 0:16] = sum_left[0:16].astype(BF)
    took(r2.at[0], s_ss.at[4], s_rs.at[4], to_left)
    sbuf[1, 0:16] = (sum_right[0:16] + r2[0].astype(F32)).astype(BF)
    go(sbuf.at[1], fin.at[0], s_ss.at[6], s_rs.at[6], to_right)
    took(r2.at[1], s_ss.at[5], s_rs.at[5], to_right)
    sbuf[2, 16:32] = (sum_left[16:32] + r2[1].astype(F32)).astype(BF)
    go(sbuf.at[2], fin.at[1], s_ss.at[7], s_rs.at[7], to_left)
    own = both(3)
    took(fin.at[0], s_ss.at[6], s_rs.at[6], to_left)
    took(fin.at[1], s_ss.at[7], s_rs.at[7], to_right)
    out_ref[...] = (own + fin[0].astype(F32) + fin[1].astype(F32)).astype(BF)
    for copy in started:
        copy.wait_send()


def output_call(o, lse, lru, lam, gain, w_lru, w_attn):
    rows, d = lru.shape[0], w_lru.shape[1]
    vm = pl.BlockSpec(memory_space=pltpu.VMEM)
    hb = pl.BlockSpec(memory_space=pl.ANY)
    dma = pltpu.SemaphoreType.DMA
    return pl.pallas_call(
        output_kernel,
        out_shape=jax.ShapeDtypeStruct((rows // 8, d), BF),
        in_specs=[vm] * 5 + [hb] * 2,
        out_specs=vm,
        scratch_shapes=[
            pltpu.VMEM((3, 2, rows, 128), BF),
            pltpu.VMEM((2, rows, 128), BF),
            pltpu.VMEM((3, 8, rows), F32),
            pltpu.VMEM((rows, 256), BF),
            pltpu.VMEM((256, d), BF),
            pltpu.VMEM((4, 2, 32, d), BF),
            pltpu.VMEM((4, 32, d), BF),
            pltpu.VMEM((3, 32, d), BF),
            pltpu.VMEM((2, 16, d), BF),
            pltpu.VMEM((2, 32, d), BF),
            dma((2,)),
            dma((9,)), dma((9,)),
            dma((8,)), dma((8,)),
        ],
        compiler_params=pltpu.CompilerParams(collective_id=2, has_side_effects=True),
        name="output",
    )(o, lse, lru, jnp.broadcast_to(lam.reshape(1, 1), (1, 128)), gain.reshape(1, 128), w_lru, w_attn)


def body(tokens, norm_gain, query_weight, w_key, w_value, w_input, w_gate, conv_kernel, w_recur, w_admit,
         decay_param, decay_scale, init_state, diff_lambda, head_gain, w_out_lru, w_out_attn):
    q, kv, lru_in, gate = project_call(tokens, norm_gain, query_weight, w_key, w_value, w_input, w_gate)
    o, lse, lru = mix_call(
        q, kv, lru_in, gate, conv_kernel, w_recur, w_admit, decay_param, decay_scale, init_state
    )
    return output_call(o, lse, lru, diff_lambda, head_gain, w_out_lru, w_out_attn)


def solution(mesh):
    torus = Mesh(
        mesh.devices.reshape(8, 8, mesh.shape["fs"], mesh.shape["tp"]), ("sp_0", "sp_1", "fs", "tp")
    )
    return jax.shard_map(
        body,
        mesh=torus,
        in_specs=(
            P(SP_FS_TP, None),
            P(),
            P(None, ("fs", "tp")),
            P(None, "tp"),
            P(None, "tp"),
            P(None, ("fs", "tp")),
            P(None, ("fs", "tp")),
            P(None, ("fs", "tp")),
            P(("fs", "tp"), None, None),
            P(("fs", "tp"), None, None),
            P(("fs", "tp")),
            P(SP, ("fs", "tp")),
            P(("fs", "tp")),
            P(("fs", "tp")),
            P(),
            P(("fs", "tp"), None),
            P(("fs", "tp"), None),
        ),
        out_specs=P(SP_FS_TP, None),
        check_vma=False,
    )
```
